32 devices in a mesh: ep: 8 (over z, core), tp: 4 (over y, x).
Axes of the slice: x: 2, y: 2, z: 4, core: 2. Of those that a mesh axis runs over, the one named last changes fastest.
Arguments:
- queries: bfloat16 [4096, 1024], P('ep', 'tp'), may hold values from -9 to 9
- keys: bfloat16 [4096, 128], P('ep'), may hold values from -6 to 6
- values: bfloat16 [4096, 128], P('ep'), may hold values from -6 to 6
- sink_logits: float32 [16], P('tp'), may hold values from 2 to 7
- out_weight: bfloat16 [1024, 2048], P(None, 'tp'), may hold values from -0.8984375 to 0.8984375
- expert_input: bfloat16 [2048, 2048], P('ep'), may hold values from -6 to 6
- norm_gain: float32 [2048], replicated, may hold values from 0.1 to 1.9
- routes: int32 [2048, 2], P('ep'), may hold values from 0 to 7, all different within a row; in each aligned block of 256 rows (0 to 255, 256 to 511, ...) at most 128 rows name the same one
- route_weights: float32 [2048, 2], P('ep'), may hold values from 0.1 to 1
- gate_weight: bfloat16 [8, 2048, 4096], P('ep', None, 'tp'), may hold values from -0.125 to 0.125
- up_weight: bfloat16 [8, 2048, 4096], P('ep', None, 'tp'), may hold values from -0.125 to 0.125
- down_weight: bfloat16 [8, 4096, 2048], P('ep', 'tp'), may hold values from -0.09375 to 0.09375
Outputs:
- attn_out: bfloat16 [4096, 2048], P('ep', 'tp')
- expert_out: bfloat16 [2048, 2048], P('ep', 'tp')
The draws below stay inside these ranges and needn't reach their ends.
Inputs may be any that keep to these rules, and one draw needn't show every extreme that they name: `routes`: each row names 2 different experts. Within the rows of one index of ep (aligned blocks of 256 rows) no expert is named by more than 128 rows, and in some blocks one expert is named by exactly 128 rows.
All inputs are finite; a program needn't handle non-finite values.
Results may differ from the reference program's by a relative error of at most 0.015.
Values may be sent and summed in bfloat16 or wider, within the bound.
A program may use at most 64 MiB of HBM per device.

```python
import math
import jax
import jax.numpy as jnp
import numpy as np
from jax import lax

D = 2048
HEADS = 16
KV = 2
HD = 64
WINDOW = 128
FF = 4096
TOPK = 2
TOK_E_DEV = 256
TOK_A = 4096
TOK_E = 2048
EXPERTS = 8
CAP = 128
N_EP = 8
N_TP = 4


def draw_queries(key, part):
    sample = jnp.clip(jax.random.normal(key, (TOK_A, HEADS * HD), jnp.float32) * 1.5, -9.0, 9.0)
    return sample.astype(jnp.bfloat16)


def draw_keys(key, part):
    sample = jnp.clip(jax.random.normal(key, (TOK_A, KV * HD), jnp.float32), -6.0, 6.0)
    return sample.astype(jnp.bfloat16)


def block_levels(key, extent, pieces, least, top_value):
    gain, own = 1.0, jax.random.fold_in(key, 6)
    for axis_at, parts in pieces:
        draws = jnp.exp(jax.random.uniform(jax.random.fold_in(own, axis_at), (parts,), jnp.float32, least / len(pieces), top_value / len(pieces)))
        gain = gain * jnp.repeat(draws, extent[axis_at] // parts).reshape([-1 if axis == axis_at else 1 for axis in range(len(extent))])
    return gain


def deal_out(key, own, number, rows, count, top, limit, lean):
    ranking = jax.random.permutation(key, count)
    packed, usual = shares(count, rows * top, limit, lean, True), shares(count, rows * top, limit, lean, False)
    places = jnp.arange(count)

    def named(lengths, turn):
        used = int((lengths > 0).sum())
        fixed = max(1, used // 4)
        moved = fixed + (places - fixed + turn * (used - fixed)) % max(1, count - fixed)
        return jnp.zeros((count,), jnp.int32).at[ranking[jnp.where(places < fixed, places, moved)]].set(jnp.asarray(lengths, jnp.int32))

    lengths = jnp.where(number % 4 == 0, named(packed, number // 4), named(usual, number - number // 4 - 1))
    mixed = jax.random.permutation(jax.random.fold_in(own, 3), count)
    source_of, receiver = mixed[0:count // 2 * 2:2], mixed[1:count // 2 * 2:2]
    margin = jnp.minimum(lengths[source_of] - 1, limit - lengths[receiver]) // 2
    margin = jnp.where((source_of == ranking[0]) | (receiver == ranking[0]) | (lengths[receiver] == 0), 0, jnp.maximum(margin, 0))
    moved = jax.random.randint(jax.random.fold_in(own, 4), (count // 2,), 0, 1 << 20) % (margin + 1)
    lengths = lengths.at[source_of].add(-moved).at[receiver].add(moved)
    members = jnp.searchsorted(jnp.cumsum(lengths), jnp.arange(rows * top), side="right").astype(jnp.int32)
    table = members.reshape(top, rows).T
    table = table[jax.random.permutation(jax.random.fold_in(own, 1), rows)]
    turn = jax.random.randint(jax.random.fold_in(own, 2), (rows, 1), 0, top)
    return jnp.take_along_axis(table, (jnp.arange(top)[None, :] + turn) % top, axis=1)


def shares(count, total, bound, slope, full):
    loads = [(1 << 20) // math.isqrt(grade ** slope) + 1 for grade in range(1, count + 1)]
    largest = bound if full else min(bound, max(-(-total // count), total * loads[0] // sum(loads)))
    least = 1 if total - largest >= count - 1 else 0
    given, rest = [largest] + [least] * (count - 1), total - largest - least * (count - 1)
    while rest > 0:
        free = [i for i in range(1, count) if given[i] < largest] or [i for i in range(1, count) if given[i] < bound]
        whole, remaining = sum([loads[i] for i in free]), rest
        for i in free:
            addition = min(bound - given[i], max(1, remaining * loads[i] // whole), rest)
            given[i] = given[i] + addition
            rest = rest - addition
    return np.array(given)


def noise(key, extent, width, most, split=(), kind=jnp.bfloat16):
    loudness = block_levels(key, extent, split, -0.22, 0.18) if split else 1.0
    values = jax.random.normal(key, extent, jnp.float32) * width * loudness
    return jnp.minimum(jnp.maximum(values, -most), most).astype(kind)


def setup_inputs(seed: int = 0) -> dict:
    streams_of = jax.random.split(jax.random.key(seed), 13)
    queries = draw_queries(jax.random.fold_in(streams_of[12], 71), 0)
    keys = draw_keys(jax.random.fold_in(streams_of[12], 71), 0)
    values = noise(streams_of[2], (TOK_A, KV * HD), 1.0, 6.0, ((0, 8),))
    sink_logits = jnp.clip(2.0 + 5.0 * jax.random.uniform(streams_of[3], (HEADS,), jnp.float32) ** block_levels(streams_of[3], (HEADS,), ((0, 4),), -0.2, 0.2), 2.0, 7.0)
    out_weight = noise(streams_of[4], (HEADS * HD, D), 0.15, 0.8984375, ((1, 4),))
    expert_input = noise(streams_of[5], (TOK_E, D), 1.0, 6.0, ((0, 8),))
    norm_gain = jnp.clip(1.0 + 0.18 * jax.random.normal(streams_of[6], (D,), jnp.float32), 0.1, 1.9)
    routes_keys = jax.random.split(jax.random.fold_in(streams_of[7], 1), TOK_E // TOK_E_DEV)
    routes_turns = jax.random.permutation(jax.random.fold_in(streams_of[7], 3), TOK_E // TOK_E_DEV)
    routes = jax.vmap(lambda own, number: deal_out(jax.random.fold_in(streams_of[7], 2), own, number, TOK_E_DEV, EXPERTS, TOPK, CAP, 1))(routes_keys, routes_turns).reshape((TOK_E, TOPK))
    route_weights = jnp.clip(0.1 + 0.9 * jax.random.uniform(streams_of[8], (TOK_E, TOPK), jnp.float32) ** block_levels(streams_of[8], (TOK_E, TOPK), ((0, 8),), -0.2, 0.2), 0.1, 1.0)
    gate_weight = noise(streams_of[9], (EXPERTS, D, FF), D ** -0.5, 0.125, ((0, 8), (2, 4)))
    up_weight = noise(streams_of[10], (EXPERTS, D, FF), D ** -0.5, 0.125, ((0, 8), (2, 4)))
    down_weight = noise(streams_of[11], (EXPERTS, FF, D), FF ** -0.5, 0.09375, ((0, 8), (1, 4)))
    return {"queries": queries, "keys": keys, "values": values, "sink_logits": sink_logits, "out_weight": out_weight, "expert_input": expert_input, "norm_gain": norm_gain, "routes": routes, "route_weights": route_weights, "gate_weight": gate_weight, "up_weight": up_weight, "down_weight": down_weight}


rms_eps = 1e-06
mask_value = -1e+30

def rotate_heads(values_in, positions):
    half_dim = values_in.shape[-1] // 2
    inv_freq = 10000.0 ** (-jnp.arange(half_dim, dtype=jnp.float32) * (2.0 / values_in.shape[-1]))
    angles = positions[:, None] * inv_freq[None, :]
    cosine_table = jnp.cos(angles)[:, None, :]
    sine_table = jnp.sin(angles)[:, None, :]
    first_half = values_in[..., :half_dim]
    second_half = values_in[..., half_dim:]
    return jnp.concatenate([first_half * cosine_table - second_half * sine_table, second_half * cosine_table + first_half * sine_table], axis=-1)

def one_head(operands):
    head_query, head_key, head_value, head_sink = operands
    tokens_all = head_query.shape[0]
    blocks = tokens_all // WINDOW
    zero_rim = jnp.zeros((WINDOW, HD), head_key.dtype)

    def band_of(source):
        padded = jnp.concatenate([zero_rim, source], axis=0)
        earlier = padded[:tokens_all].reshape(blocks, WINDOW, HD)
        current = padded[WINDOW:].reshape(blocks, WINDOW, HD)
        return jnp.concatenate([earlier, current], axis=1).astype(jnp.float32)
    query_blocks = head_query.reshape(blocks, WINDOW, HD).astype(jnp.float32)
    scores = jnp.einsum('nqd,nkd->nqk', query_blocks, band_of(head_key)) * HD ** (-0.5)
    block_start = jnp.arange(blocks, dtype=jnp.int32)[:, None, None] * WINDOW
    query_pos = block_start + jnp.arange(WINDOW, dtype=jnp.int32)[None, :, None]
    key_pos = block_start - WINDOW + jnp.arange(2 * WINDOW, dtype=jnp.int32)[None, None, :]
    distance = query_pos - key_pos
    allowed = (distance >= 0) & (distance < WINDOW) & (key_pos >= 0)
    scores = jnp.where(allowed, scores, mask_value)
    row_top = jnp.maximum(lax.optimization_barrier(jnp.max(scores, axis=-1)), head_sink)
    exp_scores = jnp.exp(scores - row_top[..., None])
    row_total = lax.optimization_barrier(jnp.sum(exp_scores, axis=-1)) + jnp.exp(head_sink - row_top)
    weights = (exp_scores / row_total[..., None]).astype(jnp.bfloat16)
    head_mix = jnp.einsum('nqk,nkd->nqd', weights.astype(jnp.float32), band_of(head_value))
    return head_mix.astype(jnp.bfloat16).reshape(tokens_all, HD)

def reference(queries, keys, values, sink_logits, out_weight, expert_input, norm_gain, routes, route_weights, gate_weight, up_weight, down_weight):
    tokens_all = queries.shape[0]
    positions = jnp.arange(tokens_all, dtype=jnp.int32).astype(jnp.float32)
    query_rot = rotate_heads(queries.astype(jnp.float32).reshape(tokens_all, HEADS, HD), positions).astype(jnp.bfloat16)
    key_rot = rotate_heads(keys.astype(jnp.float32).reshape(tokens_all, KV, HD), positions).astype(jnp.bfloat16)
    value_heads = values.reshape(tokens_all, KV, HD)
    group_size = HEADS // KV
    query_t = jnp.transpose(query_rot, (1, 0, 2))
    key_t = jnp.repeat(jnp.transpose(key_rot, (1, 0, 2)), group_size, axis=0)
    value_t = jnp.repeat(jnp.transpose(value_heads, (1, 0, 2)), group_size, axis=0)
    head_outputs = lax.map(one_head, (query_t, key_t, value_t, sink_logits.astype(jnp.float32)))
    head_mix = jnp.transpose(head_outputs, (1, 0, 2)).reshape(tokens_all, HEADS * HD)
    attn_out = jnp.dot(head_mix, out_weight, preferred_element_type=jnp.float32).astype(jnp.bfloat16)
    token_rows = expert_input.shape[0]
    input_wide = expert_input.astype(jnp.float32)
    inv_rms = lax.rsqrt(lax.optimization_barrier(jnp.mean(input_wide * input_wide, axis=-1, keepdims=True)) + rms_eps)
    normed = (input_wide * inv_rms * norm_gain.astype(jnp.float32)[None, :]).astype(jnp.bfloat16)
    grouped = routes.reshape(N_EP, TOK_E_DEV * TOPK).astype(jnp.int32)
    one_hot = (grouped[..., None] == jnp.arange(EXPERTS, dtype=jnp.int32)[None, None, :]).astype(jnp.int32)
    route_rank = lax.optimization_barrier(jnp.sum(jnp.cumsum(one_hot, axis=1) * one_hot, axis=-1)) - 1
    source_block = jnp.arange(N_EP, dtype=jnp.int32)[:, None]
    slot_index = (grouped * (N_EP * CAP) + source_block * CAP + route_rank).reshape(-1).astype(jnp.int32)
    route_token = (jnp.arange(token_rows * TOPK, dtype=jnp.int32) // TOPK).astype(jnp.int32)
    slot_table = jnp.full((EXPERTS * N_EP * CAP,), token_rows, jnp.int32).at[slot_index].set(route_token).reshape(EXPERTS, N_EP * CAP)
    padded = jnp.concatenate([normed, jnp.zeros((1, D), normed.dtype)], axis=0)
    width_block = FF // N_TP

    def one_expert(operands):
        table_row, gate_mat, up_mat, down_mat = operands
        rows_in = padded[table_row]
        gate_acc = jnp.dot(rows_in, gate_mat, preferred_element_type=jnp.float32)
        up_acc = jnp.dot(rows_in, up_mat, preferred_element_type=jnp.float32)
        hidden = (jax.nn.silu(gate_acc) * up_acc).astype(jnp.bfloat16)
        block_parts = jnp.einsum('sjf,jfd->jsd', hidden.reshape(-1, N_TP, width_block).astype(jnp.float32), down_mat.reshape(N_TP, width_block, D).astype(jnp.float32)).astype(jnp.bfloat16)
        return lax.optimization_barrier(jnp.sum(block_parts.astype(jnp.float32), axis=0)).astype(jnp.bfloat16)
    outputs = lax.map(one_expert, (slot_table, gate_weight, up_weight, down_weight))
    picked = outputs.reshape(-1, D)[slot_index].astype(jnp.float32)
    expert_out = lax.optimization_barrier(jnp.sum(picked.reshape(token_rows, TOPK, D) * route_weights.astype(jnp.float32)[..., None], axis=1)).astype(jnp.bfloat16)
    return (attn_out, expert_out)
```

```python
import jax
import jax.numpy as jnp
from jax import lax
from jax.sharding import PartitionSpec as P

HEADS = 16
KV = 2
HD = 64
WINDOW = 128


rms_eps = 1e-06
mask_value = -1e30


def passed_along(value, axis, steps):
    count = lax.axis_size(axis)
    first, last = (max(0, -steps), min(count, count - steps))
    return lax.ppermute(value, axis, [(source, source + steps) for source in range(first, last)])


def swapped(value, mask):
    count = lax.axis_size("tp")
    return lax.ppermute(value, "tp", [(source, source ^ mask) for source in range(count)])


def rotate_heads(values_in, positions):
    half_dim = values_in.shape[-1] // 2
    inv_freq = 10000.0 ** (-jnp.arange(half_dim, dtype=jnp.float32) * (2.0 / values_in.shape[-1]))
    angles = positions[:, None] * inv_freq[None, :]
    cosine_table = jnp.cos(angles)[:, None, :]
    sine_table = jnp.sin(angles)[:, None, :]
    first_half = values_in[..., :half_dim]
    second_half = values_in[..., half_dim:]
    return jnp.concatenate(
        [
            first_half * cosine_table - second_half * sine_table,
            second_half * cosine_table + first_half * sine_table,
        ],
        axis=-1,
    )


def local(
    queries,
    keys,
    values,
    sink_logits,
    out_weight,
    expert_input,
    norm_gain,
    routes,
    route_weights,
    gate_weight,
    up_weight,
    down_weight,
):
    seq_rows = queries.shape[0]
    heads_here = queries.shape[1] // HD
    group_size = HEADS // KV
    kv_here = max(1, heads_here // group_size)
    heads_per_kv = heads_here // kv_here
    kv_first = lax.axis_index("tp") * heads_here // group_size
    key_local = lax.dynamic_slice_in_dim(keys, kv_first * HD, kv_here * HD, 1)
    value_local = lax.dynamic_slice_in_dim(values, kv_first * HD, kv_here * HD, 1)
    offset = lax.axis_index("ep") * seq_rows
    positions = (offset + jnp.arange(seq_rows, dtype=jnp.int32)).astype(jnp.float32)
    query_rot = rotate_heads(
        queries.astype(jnp.float32).reshape(seq_rows, heads_here, HD), positions
    ).astype(jnp.bfloat16)
    key_rot = rotate_heads(
        key_local.astype(jnp.float32).reshape(seq_rows, kv_here, HD), positions
    ).astype(jnp.bfloat16)
    value_heads = value_local.reshape(seq_rows, kv_here, HD)
    rim_pair = jnp.concatenate(
        [
            key_rot.reshape(seq_rows, kv_here * HD)[seq_rows - WINDOW :],
            value_local[seq_rows - WINDOW :],
        ],
        axis=1,
    )
    rim_pair = passed_along(rim_pair, "ep", 1)
    rim_key = rim_pair[:, : kv_here * HD].reshape(WINDOW, kv_here, HD)
    rim_value = rim_pair[:, kv_here * HD :].reshape(WINDOW, kv_here, HD)
    blocks = seq_rows // WINDOW

    def band_of(rim_part, local_part):
        padded = jnp.concatenate([rim_part, local_part], axis=0)
        earlier = padded[:seq_rows].reshape(blocks, WINDOW, kv_here, HD)
        current = padded[WINDOW:].reshape(blocks, WINDOW, kv_here, HD)
        return jnp.concatenate([earlier, current], axis=1)

    key_band = band_of(rim_key, key_rot)
    value_band = band_of(rim_value, value_heads)
    query_blocks = query_rot.reshape(blocks, WINDOW, kv_here, heads_per_kv, HD)
    scores = jnp.einsum(
        "nqhgd,nkhd->nhgqk", query_blocks, key_band, preferred_element_type=jnp.float32
    ) * HD ** (-0.5)
    block_start = offset + jnp.arange(blocks, dtype=jnp.int32)[:, None, None] * WINDOW
    query_pos = block_start + jnp.arange(WINDOW, dtype=jnp.int32)[None, :, None]
    key_pos = block_start - WINDOW + jnp.arange(2 * WINDOW, dtype=jnp.int32)[None, None, :]
    distance = query_pos - key_pos
    allowed = (distance >= 0) & (distance < WINDOW) & (key_pos >= 0)
    scores = jnp.where(allowed[:, None, None], scores, mask_value)
    sink_row = sink_logits.reshape(1, kv_here, heads_per_kv, 1)
    row_top = jnp.maximum(jnp.max(scores, axis=-1), sink_row)
    exp_scores = jnp.exp(scores - row_top[..., None])
    row_total = jnp.sum(exp_scores, axis=-1) + jnp.exp(sink_row - row_top)
    weights = (exp_scores / row_total[..., None]).astype(jnp.bfloat16)
    head_mix = jnp.einsum(
        "nhgqk,nkhd->nqhgd", weights, value_band, preferred_element_type=jnp.float32
    )
    head_mix = head_mix.astype(jnp.bfloat16).reshape(seq_rows, heads_here * HD)
    tp_count = lax.axis_size("tp")
    square = tp_count == 4
    me_tp = lax.axis_index("tp")
    token_rows = expert_input.shape[0]
    top_count = routes.shape[1]
    expert_count = lax.axis_size("ep")
    capacity = 2 * top_count * token_rows // expert_count
    chunks = 2 if square else 1
    part_cap = capacity // chunks
    chunk_rows = expert_count * part_cap
    slot_total = expert_count * capacity
    input_wide = expert_input.astype(jnp.float32)
    inv_rms = lax.rsqrt(jnp.mean(input_wide * input_wide, axis=-1, keepdims=True) + rms_eps)
    flat_expert = routes.reshape(-1)
    one_hot = (flat_expert[:, None] == jnp.arange(expert_count, dtype=jnp.int32)[None, :]).astype(
        jnp.int32
    )
    route_rank = jnp.sum(jnp.cumsum(one_hot, axis=0) * one_hot, axis=1) - 1
    slot_of_route = (
        (route_rank // part_cap) * chunk_rows + flat_expert * part_cap + route_rank % part_cap
    )
    matches = slot_of_route[None, :] == jnp.arange(slot_total, dtype=jnp.int32)[:, None]
    route_token = jnp.arange(token_rows * top_count, dtype=jnp.int32) // top_count
    source_row = jnp.sum(jnp.where(matches, route_token[None, :], 0), axis=1)
    gate_local = gate_weight[0]
    up_local = up_weight[0]
    down_local = down_weight[0]
    column_count = expert_input.shape[1] // tp_count
    own_input = lax.dynamic_slice_in_dim(expert_input, me_tp * column_count, column_count, 1)
    own_gain = lax.dynamic_slice_in_dim(norm_gain, me_tp * column_count, column_count, 0)
    own_columns = (own_input.astype(jnp.float32) * inv_rms * own_gain[None, :]).astype(jnp.bfloat16)
    slot_rows = jnp.take(own_columns, source_row, axis=0, mode="clip")
    outgoing = slot_rows.reshape(chunks, expert_count, part_cap, column_count)
    arrived = [
        lax.all_to_all(outgoing[c], "ep", split_axis=0, concat_axis=0, tiled=True).reshape(
            chunk_rows, column_count
        )
        for c in range(chunks)
    ]

    def block_of(weight, mask, axis, width):
        return lax.dynamic_slice_in_dim(weight, (me_tp ^ mask) * width, width, axis)

    def dot(left, right):
        return jnp.dot(left, right, preferred_element_type=jnp.float32)

    summed = []
    half = chunk_rows // 2
    for c in range(chunks):
        piece = arrived[c]
        if square:
            by_x, by_y = swapped(piece, 1), swapped(piece, 2)
            far = jnp.concatenate([swapped(by_x[:half], 2), swapped(by_y[half:], 1)], axis=0)
            gate_acc, up_acc = 0.0, 0.0
            for mask, rows in ((0, piece), (1, by_x), (2, by_y), (3, far)):
                gate_acc = gate_acc + dot(rows, block_of(gate_local, mask, 0, column_count))
                up_acc = up_acc + dot(rows, block_of(up_local, mask, 0, column_count))
        else:
            rows = lax.all_gather(piece, "tp", axis=1, tiled=True)
            gate_acc, up_acc = dot(rows, gate_local), dot(rows, up_local)
        hidden = (jax.nn.silu(gate_acc) * up_acc).astype(jnp.bfloat16)
        if square:
            done = []
            for part, (first, second) in enumerate(((1, 2), (2, 1))):
                rows = hidden[part * half : (part + 1) * half]

                def product(mask):
                    return dot(rows, block_of(down_local, mask, 1, column_count)).astype(
                        jnp.bfloat16
                    )

                sent = [swapped(product(first | second), first), swapped(product(first), first)]
                passed = product(second).astype(jnp.float32) + sent[0].astype(jnp.float32)
                kept = product(0).astype(jnp.float32) + sent[1].astype(jnp.float32)
                last = swapped(passed.astype(jnp.bfloat16), second)
                done.append((kept + last.astype(jnp.float32)).astype(jnp.bfloat16))
            total = jnp.concatenate(done, axis=0)
        else:
            total = lax.psum_scatter(
                dot(hidden, down_local).astype(jnp.bfloat16),
                "tp",
                scatter_dimension=1,
                tiled=True,
            )
        summed.append(total)

    home = []
    for total in summed:
        back = lax.all_to_all(
            total.reshape(expert_count, part_cap, column_count),
            "ep",
            split_axis=0,
            concat_axis=0,
            tiled=True,
        )
        home.append(back.reshape(chunk_rows, column_count))
    home_flat = jnp.concatenate(home, axis=0) if chunks > 1 else home[0]
    route_slots = slot_of_route.reshape(token_rows, top_count)
    combined = 0.0
    for k in range(top_count):
        picked = jnp.take(home_flat, route_slots[:, k], axis=0, mode="clip").astype(jnp.float32)
        combined = combined + picked * route_weights[:, k : k + 1]
    expert_out = combined.astype(jnp.bfloat16)

    if square:
        width = heads_here * HD
        blocks_in = [head_mix] + [swapped(head_mix, mask) for mask in (1, 2, 3)]
        attn_acc = 0.0
        for mask, rows in enumerate(blocks_in):
            attn_acc = attn_acc + dot(rows, block_of(out_weight, mask, 0, width))
    else:
        attn_acc = dot(lax.all_gather(head_mix, "tp", axis=1, tiled=True), out_weight)
    attn_out = attn_acc.astype(jnp.bfloat16)
    return (attn_out, expert_out)


def solution(mesh):
    return jax.shard_map(
        local,
        mesh=mesh,
        in_specs=(
            P("ep", "tp"),
            P("ep", None),
            P("ep", None),
            P("tp"),
            P(None, "tp"),
            P("ep", None),
            P(),
            P("ep", None),
            P("ep", None),
            P("ep", None, "tp"),
            P("ep", None, "tp"),
            P("ep", "tp", None),
        ),
        out_specs=(P("ep", "tp"), P("ep", "tp")),
        check_vma=False,
    )
```

```python
import jax
import jax.numpy as jnp
from jax import lax
from jax.sharding import PartitionSpec as P

HEADS = 16
KV = 2
HD = 64
WINDOW = 128


rms_eps = 1e-06
mask_value = -1e30


def passed_along(value, axis, steps):
    count = lax.axis_size(axis)
    first, last = (max(0, -steps), min(count, count - steps))
    return lax.ppermute(value, axis, [(source, source + steps) for source in range(first, last)])


def swapped(value, mask):
    count = lax.axis_size("tp")
    return lax.ppermute(value, "tp", [(source, source ^ mask) for source in range(count)])


def held_until(value, *others):
    return lax.optimization_barrier((value, others))[0]


def rotate_heads(values_in, positions):
    half_dim = values_in.shape[-1] // 2
    inv_freq = 10000.0 ** (-jnp.arange(half_dim, dtype=jnp.float32) * (2.0 / values_in.shape[-1]))
    angles = positions[:, None] * inv_freq[None, :]
    cosine_table = jnp.cos(angles)[:, None, :]
    sine_table = jnp.sin(angles)[:, None, :]
    first_half = values_in[..., :half_dim]
    second_half = values_in[..., half_dim:]
    return jnp.concatenate(
        [
            first_half * cosine_table - second_half * sine_table,
            second_half * cosine_table + first_half * sine_table,
        ],
        axis=-1,
    )


def local(
    queries,
    keys,
    values,
    sink_logits,
    out_weight,
    expert_input,
    norm_gain,
    routes,
    route_weights,
    gate_weight,
    up_weight,
    down_weight,
):
    seq_rows = queries.shape[0]
    heads_here = queries.shape[1] // HD
    group_size = HEADS // KV
    kv_here = max(1, heads_here // group_size)
    heads_per_kv = heads_here // kv_here
    kv_first = lax.axis_index("tp") * heads_here // group_size
    key_local = lax.dynamic_slice_in_dim(keys, kv_first * HD, kv_here * HD, 1)
    value_local = lax.dynamic_slice_in_dim(values, kv_first * HD, kv_here * HD, 1)
    offset = lax.axis_index("ep") * seq_rows
    positions = (offset + jnp.arange(seq_rows, dtype=jnp.int32)).astype(jnp.float32)
    query_rot = rotate_heads(
        queries.astype(jnp.float32).reshape(seq_rows, heads_here, HD), positions
    ).astype(jnp.bfloat16)
    key_rot = rotate_heads(
        key_local.astype(jnp.float32).reshape(seq_rows, kv_here, HD), positions
    ).astype(jnp.bfloat16)
    value_heads = value_local.reshape(seq_rows, kv_here, HD)
    rim_pair = jnp.concatenate(
        [
            key_rot.reshape(seq_rows, kv_here * HD)[seq_rows - WINDOW :],
            value_local[seq_rows - WINDOW :],
        ],
        axis=1,
    )
    rim_pair = passed_along(rim_pair, "ep", 1)
    rim_key = rim_pair[:, : kv_here * HD].reshape(WINDOW, kv_here, HD)
    rim_value = rim_pair[:, kv_here * HD :].reshape(WINDOW, kv_here, HD)
    blocks = seq_rows // WINDOW

    def band_of(rim_part, local_part):
        padded = jnp.concatenate([rim_part, local_part], axis=0)
        earlier = padded[:seq_rows].reshape(blocks, WINDOW, kv_here, HD)
        current = padded[WINDOW:].reshape(blocks, WINDOW, kv_here, HD)
        return jnp.concatenate([earlier, current], axis=1)

    key_band = band_of(rim_key, key_rot)
    value_band = band_of(rim_value, value_heads)
    query_blocks = query_rot.reshape(blocks, WINDOW, kv_here, heads_per_kv, HD)
    scores = jnp.einsum(
        "nqhgd,nkhd->nhgqk", query_blocks, key_band, preferred_element_type=jnp.float32
    ) * HD ** (-0.5)
    block_start = offset + jnp.arange(blocks, dtype=jnp.int32)[:, None, None] * WINDOW
    query_pos = block_start + jnp.arange(WINDOW, dtype=jnp.int32)[None, :, None]
    key_pos = block_start - WINDOW + jnp.arange(2 * WINDOW, dtype=jnp.int32)[None, None, :]
    distance = query_pos - key_pos
    allowed = (distance >= 0) & (distance < WINDOW) & (key_pos >= 0)
    scores = jnp.where(allowed[:, None, None], scores, mask_value)
    sink_row = sink_logits.reshape(1, kv_here, heads_per_kv, 1)
    row_top = jnp.maximum(jnp.max(scores, axis=-1), sink_row)
    exp_scores = jnp.exp(scores - row_top[..., None])
    row_total = jnp.sum(exp_scores, axis=-1) + jnp.exp(sink_row - row_top)
    weights = (exp_scores / row_total[..., None]).astype(jnp.bfloat16)
    head_mix = jnp.einsum(
        "nhgqk,nkhd->nqhgd", weights, value_band, preferred_element_type=jnp.float32
    )
    head_mix = head_mix.astype(jnp.bfloat16).reshape(seq_rows, heads_here * HD)
    tp_count = lax.axis_size("tp")
    square = tp_count == 4
    me_tp = lax.axis_index("tp")
    token_rows = expert_input.shape[0]
    top_count = routes.shape[1]
    expert_count = lax.axis_size("ep")
    capacity = 2 * top_count * token_rows // expert_count
    chunks = 2 if square else 1
    part_cap = capacity // chunks
    chunk_rows = expert_count * part_cap
    slot_total = expert_count * capacity
    input_wide = expert_input.astype(jnp.float32)
    inv_rms = lax.rsqrt(jnp.mean(input_wide * input_wide, axis=-1, keepdims=True) + rms_eps)
    flat_expert = routes.reshape(-1)
    one_hot = (flat_expert[:, None] == jnp.arange(expert_count, dtype=jnp.int32)[None, :]).astype(
        jnp.int32
    )
    route_rank = jnp.sum(jnp.cumsum(one_hot, axis=0) * one_hot, axis=1) - 1
    slot_of_route = (
        (route_rank // part_cap) * chunk_rows + flat_expert * part_cap + route_rank % part_cap
    )
    matches = slot_of_route[None, :] == jnp.arange(slot_total, dtype=jnp.int32)[:, None]
    route_token = jnp.arange(token_rows * top_count, dtype=jnp.int32) // top_count
    source_row = jnp.sum(jnp.where(matches, route_token[None, :], 0), axis=1)
    gate_local = gate_weight[0]
    up_local = up_weight[0]
    down_local = down_weight[0]
    column_count = expert_input.shape[1] // tp_count
    own_input = lax.dynamic_slice_in_dim(expert_input, me_tp * column_count, column_count, 1)
    own_gain = lax.dynamic_slice_in_dim(norm_gain, me_tp * column_count, column_count, 0)
    own_columns = (own_input.astype(jnp.float32) * inv_rms * own_gain[None, :]).astype(jnp.bfloat16)
    slot_rows = jnp.take(own_columns, source_row, axis=0, mode="clip")
    outgoing = slot_rows.reshape(chunks, expert_count, part_cap, column_count)
    arrived = [
        lax.all_to_all(outgoing[c], "ep", split_axis=0, concat_axis=0, tiled=True).reshape(
            chunk_rows, column_count
        )
        for c in range(chunks)
    ]

    def block_of(weight, mask, axis, width):
        return lax.dynamic_slice_in_dim(weight, (me_tp ^ mask) * width, width, axis)

    def dot(left, right):
        return jnp.dot(left, right, preferred_element_type=jnp.float32)

    half = chunk_rows // 2

    def gather(piece):
        by_x, by_y = swapped(piece, 1), swapped(piece, 2)
        far = jnp.concatenate([swapped(by_x[:half], 2), swapped(by_y[half:], 1)], axis=0)
        return far, expand((0.0, 0.0), ((0, piece), (1, by_x), (2, by_y)))

    def expand(sums, blocks_of):
        gate_acc, up_acc = sums
        for mask, rows in blocks_of:
            gate_acc = gate_acc + dot(rows, block_of(gate_local, mask, 0, column_count))
            up_acc = up_acc + dot(rows, block_of(up_local, mask, 0, column_count))
        return gate_acc, up_acc

    def activated(sums):
        return (jax.nn.silu(sums[0]) * sums[1]).astype(jnp.bfloat16)

    def scatter_first(hidden):
        passed, kept, sent = [], [], []
        for part, (first, second) in enumerate(((1, 2), (2, 1))):
            rows = hidden[part * half : (part + 1) * half]

            def product(mask):
                return dot(rows, block_of(down_local, mask, 1, column_count)).astype(jnp.bfloat16)

            here = [swapped(product(first | second), first), swapped(product(first), first)]
            passed.append(product(second).astype(jnp.float32) + here[0].astype(jnp.float32))
            kept.append(product(0).astype(jnp.float32) + here[1].astype(jnp.float32))
            sent += here
        return passed, kept, sent

    def scatter_second(passed):
        return [swapped(passed[0].astype(jnp.bfloat16), 2), swapped(passed[1].astype(jnp.bfloat16), 1)]

    def joined(kept, last):
        return jnp.concatenate(
            [(k + l.astype(jnp.float32)).astype(jnp.bfloat16) for k, l in zip(kept, last)], axis=0
        )

    if square:
        far_a, sums_a = gather(arrived[0])
        hidden_a = activated(expand(sums_a, ((3, far_a),)))
        far_b, sums_b = gather(held_until(arrived[1], far_a))
        passed_a, kept_a, sent_a = scatter_first(hidden_a)
        last_a = scatter_second([held_until(p, *sums_b) for p in passed_a])
        sums_b = expand(sums_b, ((3, held_until(far_b, *sent_a)),))
        passed_b, kept_b, _ = scatter_first(held_until(activated(sums_b), *last_a))
        last_b = scatter_second(passed_b)
        summed = [joined(kept_a, [held_until(l, far_b) for l in last_a]), joined(kept_b, last_b)]
    else:
        rows = lax.all_gather(arrived[0], "tp", axis=1, tiled=True)
        hidden = activated((dot(rows, gate_local), dot(rows, up_local)))
        summed = [
            lax.psum_scatter(
                dot(hidden, down_local).astype(jnp.bfloat16),
                "tp",
                scatter_dimension=1,
                tiled=True,
            )
        ]

    home = []
    for total in summed:
        back = lax.all_to_all(
            total.reshape(expert_count, part_cap, column_count),
            "ep",
            split_axis=0,
            concat_axis=0,
            tiled=True,
        )
        home.append(back.reshape(chunk_rows, column_count))
    home_flat = jnp.concatenate(home, axis=0) if chunks > 1 else home[0]
    route_slots = slot_of_route.reshape(token_rows, top_count)
    combined = 0.0
    for k in range(top_count):
        picked = jnp.take(home_flat, route_slots[:, k], axis=0, mode="clip").astype(jnp.float32)
        combined = combined + picked * route_weights[:, k : k + 1]
    expert_out = combined.astype(jnp.bfloat16)

    if square:
        width = heads_here * HD
        head_mix = held_until(head_mix, summed[-1])
        blocks_in = [head_mix] + [swapped(head_mix, mask) for mask in (1, 2, 3)]
        attn_acc = 0.0
        for mask, rows in enumerate(blocks_in):
            attn_acc = attn_acc + dot(rows, block_of(out_weight, mask, 0, width))
    else:
        attn_acc = dot(lax.all_gather(head_mix, "tp", axis=1, tiled=True), out_weight)
    attn_out = attn_acc.astype(jnp.bfloat16)
    return (attn_out, expert_out)


def solution(mesh):
    return jax.shard_map(
        local,
        mesh=mesh,
        in_specs=(
            P("ep", "tp"),
            P("ep", None),
            P("ep", None),
            P("tp"),
            P(None, "tp"),
            P("ep", None),
            P(),
            P("ep", None),
            P("ep", None),
            P("ep", None, "tp"),
            P("ep", None, "tp"),
            P("ep", "tp", None),
        ),
        out_specs=(P("ep", "tp"), P("ep", "tp")),
        check_vma=False,
    )
```
